32 devices in a mesh: grp: 2 (over x), fs: 4 (over z), tp: 4 (over y, core).
Axes of the slice: x: 2, y: 2, z: 4, core: 2. Of those that a mesh axis runs over, the one named last changes fastest.
Arguments:
- tokens: bfloat16 [960, 2048], P(('grp', 'tp')), parts along dimension 0, may hold values from -60 to 60
- route_expert: int32 [960, 4], P(('grp', 'tp')), parts along dimension 0, may hold values from 0 to 31, all different within a row; in each aligned block of 120 rows (0 to 119, 120 to 239, ...) at most 16 rows name the same one
- route_weight: float32 [960, 4], P(('grp', 'tp')), parts along dimension 0, may hold values from 0.05 to 1
- norm_gain: float32 [2048], P('tp'), may hold values from 0.1 to 1.9
- gate_train: float32 [32, 2048, 2048], P(None, 'tp', 'fs'), may hold values from -8 to 8
- up_train: float32 [32, 2048, 2048], P(None, 'tp', 'fs'), may hold values from -8 to 8
- down_train: float32 [32, 2048, 2048], P(None, 'tp', 'fs'), may hold values from -0.013671875 to 0.013671875
Outputs:
- gate_serve: bfloat16 [64, 2048, 2048], P(('grp', 'tp'), None, 'fs'), parts along dimension 0
- up_serve: bfloat16 [64, 2048, 2048], P(('grp', 'tp'), None, 'fs'), parts along dimension 0
- down_serve: bfloat16 [64, 2048, 2048], P(('grp', 'tp'), None, 'fs'), parts along dimension 0
- mixed: bfloat16 [960, 2048], P(('grp', 'tp'), 'fs'), parts along dimension 0
The draws below stay inside these ranges and needn't reach their ends.
There are 2 independent parts, one for each index of `grp`. The reference program is written for one: setup_inputs(seed, part) draws one part's arguments, and reference() takes and returns one part's arrays. A program takes and returns all parts, laid end to end along the dimension named above; an argument that names none is the same for every part. Nothing has to cross between parts.
Inputs may be any that keep to these rules, and one draw needn't show every extreme that they name: `route_expert`: each row names 4 different experts; the rows of one device name each expert at most 16 times.
All inputs are finite; a program needn't handle non-finite values.
Results may differ from the reference program's by a relative error of at most 0.0087.
Values may be sent and summed in bfloat16 or wider, within the bound.
A program may use at most 320 MiB of HBM per device.

```python
import math
import jax
import jax.numpy as jnp
import numpy as np
from jax import lax

D = 2048
FF = 2048
EXPERTS = 32
TOP = 4
TOK_DEV = 120
CAP = 16
TOKENS = 480
N_TP = 4


def draw_tokens(key, part):
    keys = jax.random.split(jax.random.fold_in(key, 11), 3)
    row_scale = jnp.exp(jax.random.uniform(keys[0], (TOKENS, 1), jnp.float32, math.log(0.3), math.log(3.0)))
    col_scale = jnp.exp(jax.random.uniform(keys[1], (1, D), jnp.float32, math.log(0.3), math.log(3.0)))
    base = jnp.clip(jax.random.normal(keys[2], (TOKENS, D), jnp.float32), -6.0, 6.0)
    return (base * row_scale * col_scale).astype(jnp.bfloat16)


def weight_columns(key, salt):
    keys = jax.random.split(jax.random.fold_in(key, salt), 2)
    scales = jnp.exp(jax.random.uniform(keys[0], (EXPERTS, 1, FF), jnp.float32, math.log(0.5), math.log(8.0)))
    base = jnp.clip(jax.random.normal(keys[1], (EXPERTS, D, FF), jnp.float32), -6.0, 6.0)
    return (base * scales * D ** (-0.5)).astype(jnp.float32)


def draw_gate_train(key, part):
    return weight_columns(key, 21)


def draw_up_train(key, part):
    return weight_columns(key, 22)


def level_of(rng, shape, cuts, low, high):
    def one(dim, parts):
        steps = jax.random.uniform(jax.random.fold_in(jax.random.fold_in(rng, 6), dim), (parts,), jnp.float32, low / len(cuts), high / len(cuts))
        return jnp.repeat(jnp.exp(steps), shape[dim] // parts).reshape((-1,) + (1,) * (len(shape) - dim - 1))

    level = one(*cuts[0])
    for cut in cuts[1:]:
        level = level * one(*cut)
    return level


def deal_out(rng, own, number, rows, number_of, top, reach, lean):
    order = jax.random.permutation(rng, number_of)
    crowded, usual = portions_of(number_of, rows * top, reach, lean, True), portions_of(number_of, rows * top, reach, lean, False)
    places = jnp.arange(number_of)

    def named(sizes, offset_by):
        used = int((sizes > 0).sum())
        fixed = max(1, used // 4)
        shifted = fixed + (places - fixed + offset_by * (used - fixed)) % max(1, number_of - fixed)
        return jnp.zeros((number_of,), jnp.int32).at[order[jnp.where(places < fixed, places, shifted)]].set(jnp.asarray(sizes, jnp.int32))

    sizes = jnp.where(number % 4 == 0, named(crowded, number // 4), named(usual, number - number // 4 - 1))
    mixed = jax.random.permutation(jax.random.fold_in(own, 3), number_of)
    giver, sink = mixed[0:number_of // 2 * 2:2], mixed[1:number_of // 2 * 2:2]
    margin = jnp.minimum(sizes[giver] - 1, reach - sizes[sink]) // 2
    margin = jnp.where((giver == order[0]) | (sink == order[0]) | (sizes[sink] == 0), 0, jnp.maximum(margin, 0))
    shifted = jax.random.randint(jax.random.fold_in(own, 4), (number_of // 2,), 0, 1 << 20) % (margin + 1)
    sizes = sizes.at[giver].add(-shifted).at[sink].add(shifted)
    labels = jnp.searchsorted(jnp.cumsum(sizes), jnp.arange(rows * top), side="right").astype(jnp.int32)
    listing = labels.reshape(top, rows).T
    listing = listing[jax.random.permutation(jax.random.fold_in(own, 1), rows)]
    offset_by = jax.random.randint(jax.random.fold_in(own, 2), (rows, 1), 0, top)
    return jnp.take_along_axis(listing, (jnp.arange(top)[None, :] + offset_by) % top, axis=1)


def portions_of(count, total, reach, slope, full):
    portions = [(1 << 20) // math.isqrt(grade ** slope) + 1 for grade in range(1, count + 1)]
    largest = reach if full else min(reach, max(-(-total // count), total * portions[0] // sum(portions)))
    least = 1 if total - largest >= count - 1 else 0
    given, surplus = [largest] + [least] * (count - 1), total - largest - least * (count - 1)
    while surplus > 0:
        movable = [i for i in range(1, count) if given[i] < largest] or [i for i in range(1, count) if given[i] < reach]
        pool, left = sum([portions[i] for i in movable]), surplus
        for i in movable:
            extra = min(reach - given[i], max(1, left * portions[i] // pool), surplus)
            given[i] = given[i] + extra
            surplus = surplus - extra
    return np.array(given)


def noise(own_key, extent, deviation, reach, cuts=(), kind=jnp.bfloat16):
    values = jax.random.normal(own_key, extent, jnp.float32) * deviation
    if len(cuts) > 0:
        values = level_of(own_key, extent, cuts, -0.22, 0.18) * values
    return jnp.clip(values, min=-reach, max=reach).astype(kind)


def setup_inputs(seed: int = 0, part: int = 0) -> dict:
    key_list = jax.random.split(jax.random.key(seed), 8)
    part_splits = jax.random.split(jax.random.fold_in(key_list[7], part), 8)
    tokens = draw_tokens(jax.random.fold_in(jax.random.fold_in(key_list[7], part), 71), part)
    route_expert_keys = jax.random.split(jax.random.fold_in(part_splits[1], 1), TOKENS // TOK_DEV)
    route_expert_turns = jax.random.permutation(jax.random.fold_in(part_splits[1], 3), TOKENS // TOK_DEV)
    route_expert = jax.vmap(lambda own, number: deal_out(jax.random.fold_in(part_splits[1], 2), own, number, TOK_DEV, EXPERTS, TOP, CAP, 2))(route_expert_keys, route_expert_turns).reshape((TOKENS, TOP))
    route_weight = jnp.clip(jnp.exp(math.log(1.0) - 2.9957323 * jax.random.uniform(part_splits[2], (TOKENS, TOP), jnp.float32) ** level_of(part_splits[2], (TOKENS, TOP), ((0, 4),), -0.2, 0.2)), 0.05, 1.0)
    norm_gain = jnp.clip(1.0 + 0.18 * jax.random.normal(key_list[3], (D,), jnp.float32), 0.1, 1.9)
    gate_train = draw_gate_train(jax.random.fold_in(key_list[7], 71), part)
    up_train = draw_up_train(jax.random.fold_in(key_list[7], 71), part)
    down_train = noise(key_list[6], (EXPERTS, FF, D), (FF * 100) ** -0.5, 0.013671875, ((1, 4), (2, 4)), jnp.float32)
    return dict(tokens=tokens, route_expert=route_expert, route_weight=route_weight, norm_gain=norm_gain, gate_train=gate_train, up_train=up_train, down_train=down_train)


def activate(gate_pre, up_pre):
    clamped = jnp.minimum(gate_pre, 7.0)
    bounded = jnp.clip(up_pre, -7.0, 7.0)
    return (clamped * jax.nn.sigmoid(1.702 * clamped) * (bounded + 1.0)).astype(jnp.bfloat16)

def reference(tokens, route_expert, route_weight, norm_gain, gate_train, up_train, down_train):
    gate_serve = (gate_train * norm_gain[None, :, None]).astype(jnp.bfloat16)
    up_serve = (up_train * norm_gain[None, :, None]).astype(jnp.bfloat16)
    down_serve = down_train.astype(jnp.bfloat16)
    floated = tokens.astype(jnp.float32)
    normed = (floated * lax.rsqrt(lax.optimization_barrier(jnp.mean(floated * floated, axis=-1, keepdims=True)) + 1e-06)).astype(jnp.bfloat16)
    flat_expert = route_expert.reshape(-1).astype(jnp.int32)
    expert_ids = jnp.arange(EXPERTS, dtype=jnp.int32)
    onehot = (flat_expert[:, None] == expert_ids[None, :]).astype(jnp.int32)
    slot_rank = lax.optimization_barrier(jnp.sum((jnp.cumsum(onehot, axis=0) - 1) * onehot, axis=1)).astype(jnp.int32)
    flat_token = (jnp.arange(TOKENS * TOP, dtype=jnp.int32) // TOP).astype(jnp.int32)
    row_table = jnp.full((EXPERTS, N_TP * CAP), TOKENS, jnp.int32).at[flat_expert, slot_rank].set(flat_token)
    padded = jnp.concatenate([normed, jnp.zeros((1, D), jnp.bfloat16)], axis=0)

    def one_expert(inputs):
        row_ids, gate_one, up_one, down_one = inputs
        gathered = padded[row_ids]
        gate_pre = jnp.dot(gathered, gate_one, preferred_element_type=jnp.float32)
        up_pre = jnp.dot(gathered, up_one, preferred_element_type=jnp.float32)
        hidden = activate(gate_pre, up_pre)
        return jnp.dot(hidden, down_one, preferred_element_type=jnp.float32).astype(jnp.bfloat16)
    expert_rows = lax.map(one_expert, (row_table, gate_serve, up_serve, down_serve))
    picked = expert_rows[flat_expert, slot_rank].reshape(TOKENS, TOP, D)
    mixed = lax.optimization_barrier(jnp.sum(route_weight[:, :, None] * picked.astype(jnp.float32), axis=1)).astype(jnp.bfloat16)
    return (gate_serve, up_serve, down_serve, mixed)
```

```python
import jax
import jax.numpy as jnp
from jax import lax
from jax.sharding import PartitionSpec as P


CAP = 16
CORES = 2
AHEAD = 3


def parts_of(per):
    return 4 if per % 4 == 0 else 1


def activate(gate_pre, up_pre):
    clamped = jnp.minimum(gate_pre, 7.0)
    bounded = jnp.clip(up_pre, -7.0, 7.0)
    return (clamped * jax.nn.sigmoid(1.702 * clamped) * (bounded + 1.0)).astype(jnp.bfloat16)


def exchange(value, axis, step):
    count = lax.axis_size(axis)
    return lax.ppermute(value, axis, [(i, i ^ step) for i in range(count)])


def gather_fs(block):
    count = lax.axis_size("fs")
    me = lax.axis_index("fs")
    width = block.shape[-1]
    whole = jnp.zeros(block.shape[:-1] + (count * width,), block.dtype)
    zeros = (0,) * (block.ndim - 1)
    for step in range(count):
        piece = block if step == 0 else exchange(block, "fs", step)
        whole = lax.dynamic_update_slice(whole, piece, zeros + ((me ^ step) * width,))
    return whole


def local(tokens, route_expert, route_weight, norm_gain, gate_train, up_train, down_train):
    n = lax.axis_size("tp")
    me = lax.axis_index("tp")
    groups = lax.axis_size("grp")
    grp = lax.axis_index("grp")
    fs_count = lax.axis_size("fs")
    experts, depth, width = gate_train.shape
    per = experts // n
    half = depth // groups
    parts = parts_of(per)
    span = per // parts
    gain = norm_gain[None, :, None]

    def weights(train, scale, first, dest, row, rows):
        piece = lax.dynamic_slice(train, (dest * per + first, row, 0), (span, rows, width))
        if scale is not None:
            piece = piece * lax.dynamic_slice(scale, (0, row, 0), (1, rows, 1))
        return piece.astype(jnp.bfloat16)

    def outgoing(train, scale, part):
        first = part * span
        return [
            weights(train, scale, first, me ^ step, 0, depth)
            if step < CORES
            else weights(train, scale, first, me ^ step, grp * half, half)
            for step in range(n)
        ]

    def blank(count):
        return jnp.zeros((count, n * depth, width), jnp.bfloat16)

    def product(rows, matrix):
        return jnp.einsum("ecd,edf->ecf", rows, matrix, preferred_element_type=jnp.float32)

    trains = (gate_train, up_train, down_train)
    scales = (gain, gain, None)
    first_sent = outgoing(gate_train, gain, 0)
    first_sent[1:], tokens, route_expert = lax.optimization_barrier(
        (first_sent[1:], tokens, route_expert)
    )

    tok_rows, features = tokens.shape
    top = route_expert.shape[1]
    floated = tokens.astype(jnp.float32)
    normed = (
        floated * lax.rsqrt(jnp.mean(floated * floated, axis=-1, keepdims=True) + 1e-06)
    ).astype(jnp.bfloat16)
    flat_expert = route_expert.reshape(-1)
    expert_ids = jnp.arange(experts, dtype=jnp.int32)
    onehot = (flat_expert[:, None] == expert_ids[None, :]).astype(jnp.int32)
    slot_rank = jnp.sum((jnp.cumsum(onehot, axis=0) - 1) * onehot, axis=1)
    slot_index = flat_expert * CAP + slot_rank
    slot_hit = slot_index[:, None] == jnp.arange(experts * CAP, dtype=jnp.int32)[None, :]
    placement = slot_hit.reshape(tok_rows, top, experts * CAP).astype(jnp.float32)
    scatter_mat = jnp.sum(placement, axis=1).astype(jnp.bfloat16)
    combine_mat = jnp.sum(placement * route_weight[:, :, None], axis=1)
    col_width = features // fs_count
    column_part = lax.dynamic_slice_in_dim(
        normed, lax.axis_index("fs") * col_width, col_width, 1
    )
    buffer = lax.dot_general(
        scatter_mat, column_part, (((0,), (0,)), ((), ())), preferred_element_type=jnp.float32
    ).astype(jnp.bfloat16).reshape(n, per, CAP, col_width)
    arrived = []
    for step in range(n):
        block = lax.dynamic_index_in_dim(buffer, me ^ step, 0, keepdims=False)
        arrived.append(block if step == 0 else exchange(block, "tp", step))
    block_in = gather_fs(jnp.concatenate(arrived, axis=1))

    serves = [None, None]
    stages = [(m, part) for m in range(3) for part in range(parts)]
    down_parts, arrivals, filled = [], [], []
    for index, (m, part) in enumerate(stages):
        held = trains[m]
        if index == 0:
            sent = first_sent
        elif index < AHEAD:
            held, sent[1:] = lax.optimization_barrier((held, sent[1:]))
        else:
            held, sent[1:], arrivals[index - AHEAD][-1] = lax.optimization_barrier(
                (held, sent[1:], arrivals[index - AHEAD][-1])
            )
        if index > 0:
            sent = outgoing(held, scales[m], part)
        here = [sent[0]]
        for step in range(1, n):
            here.append(exchange(sent[step], "tp", step))
        arrivals.append(here)
    entry = min(CORES, n - 1)
    pre = []
    for index, (m, part) in enumerate(stages):
        pieces = arrivals[index]
        done = filled[index - 1] if index > 0 else blank(per)
        if part == 0 and m > 0:
            serves[m - 1] = done
            fence = product(block_in, done)
            if index + 1 < len(stages):
                arrivals[index + 1][entry], fence = lax.optimization_barrier(
                    (arrivals[index + 1][entry], fence)
                )
            pre.append(fence)
        base = part * span if m < 2 else 0
        if m < 2:
            out = done if part > 0 or m == 0 else blank(per)
        else:
            out = blank(span)
        for step in range(CORES):
            out = lax.dynamic_update_slice(out, pieces[step], (base, (me ^ step) * depth, 0))
        late = []
        for step in range(CORES, n):
            source = (me ^ step) * depth
            out = lax.dynamic_update_slice(out, pieces[step], (base, source + grp * half, 0))
            for other, row in late:
                out = lax.dynamic_update_slice(out, other, (base, row, 0))
            late = []
            for turn in range(1, groups):
                other = exchange(pieces[step], "grp", turn)
                late.append((other, source + (grp ^ turn) * half))
        for other, row in late:
            out = lax.dynamic_update_slice(out, other, (base, row, 0))
        filled.append(out)
        if m == 2:
            down_parts.append(out)
    gate_serve, up_serve = serves
    down_serve = blank(per)
    hidden = activate(*pre)
    hidden = gather_fs(hidden)
    combine = combine_mat.reshape(tok_rows, n, per, CAP)
    mixed = jnp.zeros((tok_rows, width), jnp.float32)
    for part in range(parts):
        rows = hidden[part * span : (part + 1) * span]
        out = jnp.einsum(
            "ecf,efd->ecd", rows, down_parts[part], preferred_element_type=jnp.float32
        ).astype(jnp.bfloat16)
        back, shares = [], []
        for step in range(n):
            block = out[:, step * CAP : (step + 1) * CAP].reshape(span * CAP, width)
            back.append(block if step == 0 else exchange(block, "tp", step))
            share = lax.dynamic_slice(
                combine, (0, me ^ step, part * span, 0), (tok_rows, 1, span, CAP)
            )
            shares.append(share.reshape(tok_rows, span * CAP))
        mixed = mixed + jnp.dot(
            jnp.concatenate(shares, axis=1),
            jnp.concatenate(back, axis=0).astype(jnp.float32),
            precision=lax.Precision.HIGHEST,
        )
    for part in range(parts):
        down_serve = lax.dynamic_update_slice(down_serve, down_parts[part], (part * span, 0, 0))
    return (gate_serve, up_serve, down_serve, mixed.astype(jnp.bfloat16))


def solution(mesh):
    return jax.shard_map(
        local,
        mesh=mesh,
        in_specs=(
            P(("grp", "tp"), None),
            P(("grp", "tp"), None),
            P(("grp", "tp"), None),
            P("tp"),
            P(None, "tp", "fs"),
            P(None, "tp", "fs"),
            P(None, "tp", "fs"),
        ),
        out_specs=(
            P(("grp", "tp"), None, "fs"),
            P(("grp", "tp"), None, "fs"),
            P(("grp", "tp"), None, "fs"),
            P(("grp", "tp"), "fs"),
        ),
        check_vma=False,
    )
```
